32 devices in a mesh: sp: 8 (over z, y), tp: 4 (over x, core).
Axes of the slice: x: 2, y: 2, z: 4, core: 2. Of those that a mesh axis runs over, the one named last changes fastest.
Arguments:
- hidden_states: bfloat16 [4096, 4096], P('sp', 'tp'), may hold values from -6 to 6
- pre_gain: float32 [2, 4096], replicated, may hold values from 0.1 to 1.9
- post_gain: float32 [2, 4096], P(None, 'tp'), may hold values from 0.1 to 1.9
- w_value: bfloat16 [2, 4096, 2048], P(None, 'sp', 'tp'), may hold values from -0.09375 to 0.09375
- w_outer: bfloat16 [2, 4096, 2048], P(None, 'sp', 'tp'), may hold values from -0.09375 to 0.09375
- w_inner: bfloat16 [2, 4096, 2048], P(None, 'sp', 'tp'), may hold values from -0.09375 to 0.09375
- taps: float32 [2, 3, 2048], P(None, None, 'tp'), may hold values from -3 to 3
- w_out: bfloat16 [2, 2048, 4096], P(None, 'tp', 'sp'), as said below
Outputs:
- final_states: bfloat16 [4096, 4096], P('sp', 'tp')
The draws below stay inside these ranges and needn't reach their ends.
Inputs may be any that keep to these rules, and one draw needn't show every extreme that they name: `w_out`: independent entries; the columns fall into 8 groups of 512 consecutive columns, each group with its own scale.
All inputs are finite; a program needn't handle non-finite values.
Results may differ from the reference program's by a relative error of at most 0.024.
Values may be sent and summed in bfloat16 or wider, within the bound.
A program may use at most 128 MiB of HBM per device.

```python
import jax
import jax.numpy as jnp
from jax import lax

D = 4096
CONV = 2048
LAYERS = 2
TAPS = 3
TOKENS = 4096
N_TP = 4


def draw_w_out(key, part):
    first, second = jax.random.split(jax.random.fold_in(key, 17))
    base = jax.random.truncated_normal(first, -4.0, 4.0, (LAYERS, CONV, D), jnp.float32) * CONV ** (-0.5)
    group_scale = jnp.exp(jax.random.uniform(second, (LAYERS, 1, 8), jnp.float32, -1.2, 1.2))
    widened = jnp.repeat(group_scale, D // 8, axis=2)
    return (base * widened).astype(jnp.bfloat16)


def steps_of(stream_key, shape, cuts, least, largest):
    factor_of, own = 1.0, jax.random.fold_in(stream_key, 6)
    for dim, blocks in cuts:
        heights = jnp.exp(jax.random.uniform(jax.random.fold_in(own, dim), (blocks,), jnp.float32, least / len(cuts), largest / len(cuts)))
        factor_of = factor_of * jnp.repeat(heights, shape[dim] // blocks).reshape([-1 if axis == dim else 1 for axis in range(len(shape))])
    return factor_of


def centred(stream_key, dims, spread, reach, pieces=(), kind=jnp.bfloat16):
    entries = spread * jax.random.normal(stream_key, dims, jnp.float32)
    if pieces:
        entries = entries * steps_of(stream_key, dims, pieces, -0.22, 0.18)
    return jnp.clip(entries, -reach, reach).astype(kind)


def setup_inputs(seed: int = 0) -> dict:
    splits = jax.random.split(jax.random.key(seed), 9)
    return {
        "hidden_states": centred(splits[0], (TOKENS, D), 1.0, 6.0, ((0, 8), (1, 4))),
        "pre_gain": jnp.clip(1.0 + 0.18 * jax.random.normal(splits[1], (LAYERS, D), jnp.float32), 0.1, 1.9),
        "post_gain": jnp.clip(1.0 + 0.18 * jax.random.normal(splits[2], (LAYERS, D), jnp.float32), 0.1, 1.9),
        "w_value": centred(splits[3], (LAYERS, D, CONV), D ** -0.5, 0.09375, ((1, 8), (2, 4))),
        "w_outer": centred(splits[4], (LAYERS, D, CONV), D ** -0.5, 0.09375, ((1, 8), (2, 4))),
        "w_inner": centred(splits[5], (LAYERS, D, CONV), D ** -0.5, 0.09375, ((1, 8), (2, 4))),
        "taps": centred(splits[6], (LAYERS, TAPS, CONV), 0.58, 3.0, ((2, 4),), jnp.float32),
        "w_out": draw_w_out(jax.random.fold_in(splits[8], 71), 0),
    }


eps = 1e-06

def reference(hidden_states, pre_gain, post_gain, w_value, w_outer, w_inner, taps, w_out):
    current = hidden_states
    length = hidden_states.shape[0]
    block_width = CONV // N_TP
    for layer_index in range(LAYERS):
        widened = current.astype(jnp.float32)
        normed = (widened * lax.rsqrt(lax.optimization_barrier(jnp.mean(widened * widened, axis=1, keepdims=True)) + eps) * pre_gain[layer_index]).astype(jnp.bfloat16)
        value_proj = jnp.dot(normed, w_value[layer_index], preferred_element_type=jnp.float32)
        outer_proj = jnp.dot(normed, w_outer[layer_index], preferred_element_type=jnp.float32)
        inner_proj = jnp.dot(normed, w_inner[layer_index], preferred_element_type=jnp.float32)
        gated_input = (inner_proj * value_proj).astype(jnp.bfloat16)
        padded = jnp.pad(gated_input, ((2, 0), (0, 0))).astype(jnp.float32)
        kernel = taps[layer_index]
        convolved = padded[0:length] * kernel[0] + padded[1:length + 1] * kernel[1] + padded[2:length + 2] * kernel[2]
        conv_out = (outer_proj * convolved).astype(jnp.bfloat16)
        weight_out = w_out[layer_index]

        def add_block(block_index, total):
            begin = (block_index * block_width).astype(jnp.int32)
            columns = lax.dynamic_slice_in_dim(conv_out, begin, block_width, 1)
            rows = lax.dynamic_slice_in_dim(weight_out, begin, block_width, 0)
            partial_term = jnp.dot(columns, rows, preferred_element_type=jnp.float32).astype(jnp.bfloat16)
            partial_term = lax.optimization_barrier(partial_term)
            return total + partial_term.astype(jnp.float32)
        mixed = lax.fori_loop(0, N_TP, add_block, jnp.zeros((length, D), jnp.float32))
        rescale = lax.rsqrt(lax.optimization_barrier(jnp.mean(mixed * mixed, axis=1, keepdims=True)) + eps)
        current = (widened + mixed * rescale * post_gain[layer_index]).astype(jnp.bfloat16)
    return current
```

```python
import functools

import jax
import jax.numpy as jnp
from jax import lax
from jax.experimental import pallas as pl
from jax.experimental.pallas import tpu as pltpu
from jax.sharding import PartitionSpec as P

MESH = pl.DeviceIdType.MESH
HALO = 16
eps = 1e-06
F32 = jnp.float32
BF16 = jnp.bfloat16


def kernel(
    SP, TP, h_ref, pre, post, wv, wo, wi, taps, wout, out_ref,
    wbuf, obuf, xbuf, nbuf, pbuf, pa, pb, mixed, gbuf, oubuf, hbuf, cbuf, pw,
    own_sem, sR, rR, sL, rL, sY, rY, sX, rX, sXr, rXr, sA, rA, sB, rB, sP, rP, sH, rH, xsem,
):
    Y = TP // 2
    Z = SP // Y
    X = TP // 2
    s = lax.axis_index("sp")
    t = lax.axis_index("tp")
    z, y = s // Y, s % Y
    x, c = t // 2, t % 2
    L, Ds, Ct = wv.shape
    Tk, Dt = h_ref.shape
    D = Dt * TP
    items = 4 * L
    wrefs = (wi, wv, wo, wout)

    def rcopy(src, dst, ss, rs, dev):
        return pltpu.make_async_remote_copy(
            src_ref=src, dst_ref=dst, send_sem=ss, recv_sem=rs, device_id=dev, device_id_type=MESH
        )

    barrier = pltpu.get_barrier_semaphore()

    def hello(dev):
        pl.semaphore_signal(barrier, inc=1, device_id=dev, device_id_type=MESH)

    for by in (Y, SP - Y, 1, SP - 1):
        hello(((s + by) % SP, t))
    for d in range(1, Y):
        hello((z * Y + (y + d) % Y, t))
    for d in range(1, TP):
        hello((s, (t + d) % TP))
    pl.semaphore_wait(barrier, 4 + Y - 1 + TP - 1)

    def slot(i, b):
        l, m = divmod(i, 4)
        if m < 3:
            return wbuf.at[l, m, pl.ds(pl.multiple_of(b * Ds, Ds), Ds)]
        return obuf.at[l, pl.ds(pl.multiple_of(b * Ct, Ct), Ct)]

    def own(i):
        l, m = divmod(i, 4)
        return wrefs[m].at[l]

    def to_right(i, h, src=None):
        b = slot(i, (z - h) * Y + y)
        return rcopy(b if src is None else src, b, sR.at[i, h], rR.at[i, h], (s + Y, t))

    def to_left(i, h, src=None):
        b = slot(i, (z + h) * Y + y)
        return rcopy(b if src is None else src, b, sL.at[i, h], rL.at[i, h], (s - Y, t))

    def from_left(i, h):
        b = slot(i, (z - 1 - h) * Y + y)
        return rcopy(b, b, sR.at[i, h], rR.at[i, h], (s - Y, t))

    def from_right(i, h):
        b = slot(i, (z + 1 + h) * Y + y)
        return rcopy(b, b, sL.at[i, h], rL.at[i, h], (s + Y, t))

    def across(i, zb, d, src=None):
        b = slot(i, zb * Y + y)
        return rcopy(
            b if src is None else src, b, sY.at[i, zb, d - 1], rY.at[i, zb, d - 1],
            (z * Y + (y + d) % Y, t),
        )

    def from_across(i, zb, d):
        b = slot(i, zb * Y + (y - d + Y) % Y)
        return rcopy(b, b, sY.at[i, zb, d - 1], rY.at[i, zb, d - 1], (z * Y + (y + d) % Y, t))

    def own_copy(i):
        return pltpu.make_async_copy(own(i), slot(i, s), own_sem.at[i])

    def stage(i, h):
        if h == 0:
            @pl.when(z < Z - 1)
            def _():
                to_right(i, 0, own(i)).start()

            @pl.when(z > 0)
            def _():
                to_left(i, 0, own(i)).start()

            for d in range(1, Y):
                across(i, z, d, own(i)).start()
            own_copy(i).start()
            return

        @pl.when(z - h >= 0)
        def _():
            from_left(i, h - 1).wait_recv()
            if h <= Z - 2:
                @pl.when(z < Z - 1)
                def _():
                    to_right(i, h).start()
            for d in range(1, Y):
                across(i, z - h, d).start()

        @pl.when(z + h <= Z - 1)
        def _():
            from_right(i, h - 1).wait_recv()
            if h <= Z - 2:
                @pl.when(z > 0)
                def _():
                    to_left(i, h).start()
            for d in range(1, Y):
                across(i, z + h, d).start()

    def advance(tau):
        for i in range(items):
            if 0 <= tau - i <= Z - 1:
                stage(i, tau - i)

    def arrived(i):
        own_copy(i).wait()
        for zb in range(Z):
            for d in range(1, Y):
                from_across(i, zb, d).wait_recv()

    mate = (s, x * 2 + 1 - c)

    def x_mate(l, src):
        return rcopy(src, xbuf.at[t], sX.at[l, 0], rX.at[l, 0], mate)

    def x_far(l, dx, src):
        return rcopy(src, xbuf.at[t], sX.at[l, dx], rX.at[l, dx], (s, ((x + dx) % X) * 2 + c))

    def x_relay(l, dx):
        b = xbuf.at[((x - dx + X) % X) * 2 + c]
        return rcopy(b, b, sXr.at[l, dx], rXr.at[l, dx], mate)

    def gather_start(l, src):
        for dx in range(1, X):
            x_far(l, dx, src).start()
        x_mate(l, src).start()

    def gather_end(l, src):
        for dx in range(1, X):
            b = xbuf.at[((x - dx + X) % X) * 2 + c]
            rcopy(b, b, sX.at[l, dx], rX.at[l, dx], mate).wait_recv()
            x_relay(l, dx).start()
        b = xbuf.at[x * 2 + 1 - c]
        rcopy(b, b, sX.at[l, 0], rX.at[l, 0], mate).wait_recv()
        for dx in range(1, X):
            b = xbuf.at[((x - dx + X) % X) * 2 + 1 - c]
            rcopy(b, b, sXr.at[l, dx], rXr.at[l, dx], mate).wait_recv()
        x_mate(l, src).wait_send()
        for dx in range(1, X):
            x_far(l, dx, src).wait_send()
            x_relay(l, dx).wait_send()

    rows = 128 if Tk % 128 == 0 else Tk

    def norm(l):
        @pl.loop(0, Tk // rows)
        def _(r):
            at = pl.ds(pl.multiple_of(r * rows, rows), rows)
            total = jnp.zeros((rows, 1), F32)
            for k in range(TP):
                v = xbuf[k, at, :].astype(F32)
                total += jnp.sum(v * v, axis=1, keepdims=True)
            scale = lax.rsqrt(total / D + eps)
            for k in range(TP):
                cols = slice(k * Dt, (k + 1) * Dt)
                v = xbuf[k, at, :].astype(F32)
                nbuf[at, cols] = (v * scale * pre[l : l + 1, cols]).astype(BF16)

    tile = 256 if Ct % 256 == 0 else Ct

    def up(l):
        @pl.loop(0, Ct // tile)
        def _(j):
            cols = pl.ds(pl.multiple_of(j * tile, tile), tile)
            inner = jnp.dot(nbuf[...], wbuf[l, 0, :, cols], preferred_element_type=F32)
            value = jnp.dot(nbuf[...], wbuf[l, 1, :, cols], preferred_element_type=F32)
            gbuf[:, cols] = (inner * value).astype(BF16)
            oubuf[:, cols] = jnp.dot(nbuf[...], wbuf[l, 2, :, cols], preferred_element_type=F32)

    def halo(l, dev):
        return rcopy(gbuf.at[pl.ds(Tk - HALO, HALO)], hbuf.at[l], sH.at[l], rH.at[l], dev)

    def conv(l):
        @pl.when(s < SP - 1)
        def _():
            halo(l, (s + 1, t)).start()

        @pl.when(s > 0)
        def _():
            halo(l, (s - 1, t)).wait_recv()

        @pl.when(s == 0)
        def _():
            hbuf[l] = jnp.zeros((HALO, Ct), BF16)

        @pl.loop(0, Ct // 128)
        def _(j):
            cols = pl.ds(pl.multiple_of(j * 128, 128), 128)
            g = gbuf[:, cols].astype(F32)
            before = hbuf[l, :, cols].astype(F32)
            last, prev = before[HALO - 1 : HALO, :], before[HALO - 2 : HALO - 1, :]
            at = lax.broadcasted_iota(jnp.int32, g.shape, 0)
            g1 = jnp.where(at == 0, last, pltpu.roll(g, 1, 0))
            g2 = jnp.where(at == 0, prev, jnp.where(at == 1, last, pltpu.roll(g, 2, 0)))
            conv = g2 * taps[l, 0:1, cols] + g1 * taps[l, 1:2, cols] + g * taps[l, 2:3, cols]
            cbuf[:, cols] = (oubuf[:, cols] * conv).astype(BF16)

        @pl.when(s < SP - 1)
        def _():
            halo(l, (s + 1, t)).wait_send()

    nb = Dt // Ds

    def out_block(l, k):
        for b in range(nb):
            at = pl.ds(pl.multiple_of((k * nb + b) * Ct, Ct), Ct)
            pbuf[k, :, b * Ds : (b + 1) * Ds] = jnp.dot(
                cbuf[...], obuf[l, at, :], preferred_element_type=F32
            ).astype(BF16)

    def send_a(l, xx):
        return rcopy(pbuf.at[xx * 2 + 1 - c], pa.at[xx], sA.at[l, xx], rA.at[l, xx], mate)

    def send_b(l, dx):
        xx = (x + dx) % X
        return rcopy(pbuf.at[xx * 2 + c], pb.at[dx - 1], sB.at[l, dx], rB.at[l, dx], (s, xx * 2 + c))

    def send_p(l, d):
        return rcopy(pw.at[0], pw.at[d], sP.at[l, d], rP.at[l, d], (s, (t + d) % TP))

    def down(l):
        for dx in range(1, X + 1):
            xx = (x + dx) % X
            out_block(l, xx * 2 + 1 - c)
            send_a(l, xx).start()
        for dx in range(1, X):
            xx = (x + dx) % X
            k = xx * 2 + c
            out_block(l, k)
            send_a(l, xx).wait_recv()

            @pl.loop(0, Tk // rows)
            def _(r):
                at = pl.ds(pl.multiple_of(r * rows, rows), rows)
                pbuf[k, at, :] = (pbuf[k, at, :].astype(F32) + pa[xx, at, :].astype(F32)).astype(BF16)

            send_b(l, dx).start()
        out_block(l, t)

    def finish(l):
        send_a(l, x).wait_recv()
        for dx in range(1, X):
            send_b(l, dx).wait_recv()

        @pl.loop(0, Tk // rows)
        def _(r):
            at = pl.ds(pl.multiple_of(r * rows, rows), rows)
            total = pbuf[t, at, :].astype(F32) + pa[x, at, :].astype(F32)
            for dx in range(1, X):
                total += pb[dx - 1, at, :].astype(F32)
            mixed[at, :] = total
            power = jnp.sum(total * total, axis=1, keepdims=True)
            pw[0, :, at] = jnp.transpose(jnp.broadcast_to(power, (rows, 128)))[0:8, :]

        for d in range(1, TP):
            send_p(l, d).start()
        for d in range(1, TP):
            send_p(l, d).wait_recv()
        for d in range(1, TP):
            send_p(l, d).wait_send()
        for xx in range(X):
            send_a(l, xx).wait_send()
        for dx in range(1, X):
            send_b(l, dx).wait_send()

        @pl.loop(0, Tk // rows)
        def _(r):
            at = pl.ds(pl.multiple_of(r * rows, rows), rows)
            power = pw[0, :, at]
            for d in range(1, TP):
                power += pw[d, :, at]
            power = jnp.transpose(jnp.broadcast_to(power[0:1, :], (128, rows)))[:, 0:1]
            scale = lax.rsqrt(power / D + eps)
            new = xbuf[t, at, :].astype(F32) + mixed[at, :] * scale * post[l : l + 1, :]
            if l == L - 1:
                out_ref[at, :] = new.astype(BF16)
            else:
                xbuf[t, at, :] = new.astype(BF16)

    first = pltpu.make_async_copy(h_ref, xbuf.at[t], xsem)
    first.start()
    tau = 0
    advance(tau)
    gather_start(0, h_ref)
    last_tau = items - 1 + Z - 1

    def advance_to(upto):
        nonlocal tau
        while tau < min(upto, last_tau):
            tau += 1
            advance(tau)

    advance_to(2)
    first.wait()
    gather_end(0, h_ref)
    norm(0)
    for l in range(L):
        base = 4 * l
        advance_to(base + 2 + Z - 1)
        for m in range(3):
            arrived(base + m)
        up(l)
        conv(l)
        advance_to(base + 3 + Z - 1)
        arrived(base + 3)
        down(l)
        advance_to(base + 4 + Z - 1)
        finish(l)
        if l < L - 1:
            gather_start(l + 1, xbuf.at[t])
            advance_to(base + 5 + Z - 1)
            gather_end(l + 1, xbuf.at[t])
            norm(l + 1)

    for i in range(items):
        for h in range(Z - 1):
            @pl.when((z < Z - 1) & (z - h >= 0))
            def _():
                to_right(i, h).wait_send()

            @pl.when((z > 0) & (z + h <= Z - 1))
            def _():
                to_left(i, h).wait_send()

        for zb in range(Z):
            for d in range(1, Y):
                across(i, zb, d).wait_send()


def solution(mesh):
    SP, TP = mesh.shape["sp"], mesh.shape["tp"]

    def local(hidden_states, pre_gain, post_gain, w_value, w_outer, w_inner, taps, w_out):
        Tk, Dt = hidden_states.shape
        L, Ds, Ct = w_value.shape
        X = Y = TP // 2
        Z = SP // Y
        items = 4 * L
        dma = pltpu.SemaphoreType.DMA
        vmem = pl.BlockSpec(memory_space=pltpu.VMEM)
        hbm = pl.BlockSpec(memory_space=pltpu.HBM)
        return pl.pallas_call(
            functools.partial(kernel, SP, TP),
            out_shape=jax.ShapeDtypeStruct((Tk, Dt), BF16),
            in_specs=[hbm, vmem, vmem, hbm, hbm, hbm, vmem, hbm],
            out_specs=vmem,
            scratch_shapes=[
                pltpu.VMEM((L, 3, SP * Ds, Ct), BF16),
                pltpu.VMEM((L, SP * Ct, Ds), BF16),
                pltpu.VMEM((TP, Tk, Dt), BF16),
                pltpu.VMEM((Tk, Dt * TP), BF16),
                pltpu.VMEM((TP, Tk, Dt), BF16),
                pltpu.VMEM((X, Tk, Dt), BF16),
                pltpu.VMEM((max(X - 1, 1), Tk, Dt), BF16),
                pltpu.VMEM((Tk, Dt), F32),
                pltpu.VMEM((Tk, Ct), BF16),
                pltpu.VMEM((Tk, Ct), F32),
                pltpu.VMEM((L, HALO, Ct), BF16),
                pltpu.VMEM((Tk, Ct), BF16),
                pltpu.VMEM((TP, 8, Tk), F32),
                dma((items,)),
                dma((items, Z)), dma((items, Z)),
                dma((items, Z)), dma((items, Z)),
                dma((items, Z, Y)), dma((items, Z, Y)),
                dma((L, X)), dma((L, X)),
                dma((L, X)), dma((L, X)),
                dma((L, X)), dma((L, X)),
                dma((L, X)), dma((L, X)),
                dma((L, TP)), dma((L, TP)),
                dma((L,)), dma((L,)),
                dma,
            ],
            compiler_params=pltpu.CompilerParams(
                collective_id=0, has_side_effects=True, vmem_limit_bytes=67043328
            ),
        )(hidden_states, pre_gain, post_gain, w_value, w_outer, w_inner, taps, w_out)

    placed = (
        P("sp", "tp"),
        P(),
        P(None, "tp"),
        P(None, "sp", "tp"),
        P(None, "sp", "tp"),
        P(None, "sp", "tp"),
        P(None, None, "tp"),
        P(None, "tp", "sp"),
    )
    return jax.shard_map(
        local, mesh=mesh, in_specs=placed, out_specs=P("sp", "tp"), check_vma=False
    )
```

```python
import functools

import jax
import jax.numpy as jnp
from jax import lax
from jax.experimental import pallas as pl
from jax.experimental.pallas import tpu as pltpu
from jax.sharding import PartitionSpec as P

MESH = pl.DeviceIdType.MESH
HALO = 16
eps = 1e-06
F32 = jnp.float32
BF16 = jnp.bfloat16


def layout(SP, TP, Ct):
    Y = 2 if SP % 2 == 0 and Ct % 256 == 0 else 1
    return Y, SP // Y, TP // 2


def kernel(
    SP, TP, h_ref, pre, post, wv, wo, wi, taps, wout, out_ref,
    wbuf, obuf, xbuf, nbuf, pbuf, pa, pb, mixed, gbuf, oubuf, hbuf, cbuf, pw,
    own_sem, sR, rR, sL, rL, sY, rY, sX, rX, sXr, rXr, sA, rA, sB, rB, sP, rP, sH, rH, xsem,
):
    Y, Z, X = layout(SP, TP, wv.shape[2])
    G = Y * X
    s = lax.axis_index("sp")
    t = lax.axis_index("tp")
    z, y = s // Y, s % Y
    x, c = t // 2, t % 2
    L, Ds, Ct = wv.shape
    Cv = Ct // Y
    Tk, Dt = h_ref.shape
    g = y * X + x
    D = Dt * TP
    items = 4 * L
    wrefs = (wi, wv, wo, wout)

    def rcopy(src, dst, ss, rs, dev):
        return pltpu.make_async_remote_copy(
            src_ref=src, dst_ref=dst, send_sem=ss, recv_sem=rs, device_id=dev, device_id_type=MESH
        )

    barrier = pltpu.get_barrier_semaphore()

    def hello(dev):
        pl.semaphore_signal(barrier, inc=1, device_id=dev, device_id_type=MESH)

    for by in (Y, SP - Y):
        hello(((s + by) % SP, t))
    for dy in range(Y):
        for d in range(TP):
            if dy or d:
                hello((z * Y + (y + dy) % Y, (t + d) % TP))
    pl.semaphore_wait(barrier, 2 + Y * TP - 1)

    def slot(i, b, n):
        l, m = divmod(i, 4)
        if m < 3:
            return wbuf.at[l, m, pl.ds(pl.multiple_of(b * Ds, Ds), n * Ds)]
        return obuf.at[l, pl.ds(pl.multiple_of(b * Cv, Cv), n * Cv)]

    def part(i, yy):
        l, m = divmod(i, 4)
        at = pl.ds(pl.multiple_of(yy * Cv, Cv), Cv)
        return wrefs[m].at[l, :, at] if m < 3 else wrefs[m].at[l, at]

    def to_right(i, h):
        b = slot(i, (z - h) * Y, Y)
        return rcopy(b, b, sR.at[i, h], rR.at[i, h], (s + Y, t))

    def to_left(i, h):
        b = slot(i, (z + h) * Y, Y)
        return rcopy(b, b, sL.at[i, h], rL.at[i, h], (s - Y, t))

    def from_left(i, h):
        b = slot(i, (z - 1 - h) * Y, Y)
        return rcopy(b, b, sR.at[i, h], rR.at[i, h], (s - Y, t))

    def from_right(i, h):
        b = slot(i, (z + 1 + h) * Y, Y)
        return rcopy(b, b, sL.at[i, h], rL.at[i, h], (s + Y, t))

    def across(i, d):
        yy = (y + d) % Y
        return rcopy(part(i, yy), slot(i, s, 1), sY.at[i, d], rY.at[i, d], (z * Y + yy, t))

    def from_across(i, d):
        b = slot(i, z * Y + (y - d + Y) % Y, 1)
        return rcopy(b, b, sY.at[i, d], rY.at[i, d], (z * Y + (y + d) % Y, t))

    def own_copy(i):
        return pltpu.make_async_copy(part(i, y), slot(i, s, 1), own_sem.at[i])

    def exchange(i):
        own_copy(i).start()
        for d in range(1, Y):
            across(i, d).start()

    def stage(i, h):
        if h == 0:
            own_copy(i).wait()
            for d in range(1, Y):
                from_across(i, d).wait_recv()

            @pl.when(z < Z - 1)
            def _():
                to_right(i, 0).start()

            @pl.when(z > 0)
            def _():
                to_left(i, 0).start()

            return

        @pl.when(z - h >= 0)
        def _():
            from_left(i, h - 1).wait_recv()
            if h <= Z - 2:
                @pl.when(z < Z - 1)
                def _():
                    to_right(i, h).start()

        @pl.when(z + h <= Z - 1)
        def _():
            from_right(i, h - 1).wait_recv()
            if h <= Z - 2:
                @pl.when(z > 0)
                def _():
                    to_left(i, h).start()

    begins = [min(i, items - 2) for i in range(items)]

    def advance(tau):
        for i in range(items):
            if 0 <= tau - begins[i] <= Z - 1:
                stage(i, tau - begins[i])

    mate = (s, x * 2 + 1 - c)

    def dev(gg, cc):
        return (z * Y + gg // X, (gg % X) * 2 + cc)

    me = g * 2 + c

    def x_mate(l, src):
        return rcopy(src, xbuf.at[me], sX.at[l, 0], rX.at[l, 0], mate)

    def x_far(l, d, src):
        return rcopy(src, xbuf.at[me], sX.at[l, d], rX.at[l, d], dev((g + d) % G, c))

    def x_relay(l, d):
        b = xbuf.at[((g - d + G) % G) * 2 + c]
        return rcopy(b, b, sXr.at[l, d], rXr.at[l, d], mate)

    def gather_start(l, src):
        for d in range(1, G):
            x_far(l, d, src).start()
        x_mate(l, src).start()

    def gather_end(l, src, between):
        for d in range(1, G):
            b = xbuf.at[((g - d + G) % G) * 2 + c]
            rcopy(b, b, sX.at[l, d], rX.at[l, d], mate).wait_recv()
            x_relay(l, d).start()
            if d == 1:
                between()
        b = xbuf.at[g * 2 + 1 - c]
        rcopy(b, b, sX.at[l, 0], rX.at[l, 0], mate).wait_recv()
        for d in range(1, G):
            b = xbuf.at[((g - d + G) % G) * 2 + 1 - c]
            rcopy(b, b, sXr.at[l, d], rXr.at[l, d], mate).wait_recv()
        x_mate(l, src).wait_send()
        for d in range(1, G):
            x_far(l, d, src).wait_send()
            x_relay(l, d).wait_send()

    rows = 128 if Tk % 128 == 0 else Tk

    def norm(l):
        for yy in range(Y):
            @pl.loop(0, Tk // rows)
            def _(r):
                at = pl.ds(pl.multiple_of(r * rows, rows), rows)
                to = pl.ds(pl.multiple_of(yy * Tk + r * rows, rows), rows)
                total = jnp.zeros((rows, 1), F32)
                for k in range(TP):
                    v = xbuf[yy * TP + k, at, :].astype(F32)
                    total += jnp.sum(v * v, axis=1, keepdims=True)
                scale = lax.rsqrt(total / D + eps)
                for k in range(TP):
                    cols = slice(k * Dt, (k + 1) * Dt)
                    v = xbuf[yy * TP + k, at, :].astype(F32)
                    nbuf[to, cols] = (v * scale * pre[l : l + 1, cols]).astype(BF16)

    def up(l):
        @pl.loop(0, Y)
        def _(j):
            at = pl.ds(pl.multiple_of(j * Tk, Tk), Tk)
            inner = jnp.dot(nbuf[at, :], wbuf[l, 0], preferred_element_type=F32)
            value = jnp.dot(nbuf[at, :], wbuf[l, 1], preferred_element_type=F32)
            gbuf[at, :] = (inner * value).astype(BF16)
            oubuf[at, :] = jnp.dot(nbuf[at, :], wbuf[l, 2], preferred_element_type=F32)

    def halo(l, dev):
        return rcopy(gbuf.at[pl.ds(Y * Tk - HALO, HALO)], hbuf.at[l], sH.at[l], rH.at[l], dev)

    def conv(l):
        @pl.when(z < Z - 1)
        def _():
            halo(l, (s + Y, t)).start()

        @pl.when(z > 0)
        def _():
            halo(l, (s - Y, t)).wait_recv()

        @pl.when(z == 0)
        def _():
            hbuf[l] = jnp.zeros((HALO, Cv), BF16)

        @pl.loop(0, Cv // 128)
        def _(j):
            cols = pl.ds(pl.multiple_of(j * 128, 128), 128)
            mine = pl.ds(pl.multiple_of(y * Cv + j * 128, 128), 128)
            v = gbuf[:, cols].astype(F32)
            before = hbuf[l, :, cols].astype(F32)
            last, prev = before[HALO - 1 : HALO, :], before[HALO - 2 : HALO - 1, :]
            at = lax.broadcasted_iota(jnp.int32, v.shape, 0)
            g1 = jnp.where(at == 0, last, pltpu.roll(v, 1, 0))
            g2 = jnp.where(at == 0, prev, jnp.where(at == 1, last, pltpu.roll(v, 2, 0)))
            conv = g2 * taps[l, 0:1, mine] + g1 * taps[l, 1:2, mine] + v * taps[l, 2:3, mine]
            cbuf[:, cols] = (oubuf[:, cols] * conv).astype(BF16)

        @pl.when(z < Z - 1)
        def _():
            halo(l, (s + Y, t)).wait_send()

    nb = Dt // Ds

    def out_block(l, gg, cc):
        yy, tt = gg // X, (gg % X) * 2 + cc
        at = pl.ds(pl.multiple_of(yy * Tk, Tk), Tk)
        for b in range(nb):
            of = pl.ds(pl.multiple_of((tt * nb + b) * Cv, Cv), Cv)
            pbuf[gg * 2 + cc, :, b * Ds : (b + 1) * Ds] = jnp.dot(
                cbuf[at, :], obuf[l, of, :], preferred_element_type=F32
            ).astype(BF16)

    def send_a(l, xx):
        return rcopy(pbuf.at[xx * 2 + 1 - c], pa.at[xx], sA.at[l, xx], rA.at[l, xx], mate)

    def send_b(l, dx):
        gg = (g + dx) % G
        return rcopy(pbuf.at[gg * 2 + c], pb.at[dx - 1], sB.at[l, dx], rB.at[l, dx], dev(gg, c))

    def send_p(l, d):
        return rcopy(pw.at[0], pw.at[d], sP.at[l, d], rP.at[l, d], (s, (t + d) % TP))

    def down(l):
        for dx in range(1, G + 1):
            xx = (g + dx) % G
            out_block(l, xx, 1 - c)
            send_a(l, xx).start()
        for dx in range(1, G):
            xx = (g + dx) % G
            k = xx * 2 + c
            out_block(l, xx, c)
            send_a(l, xx).wait_recv()

            @pl.loop(0, Tk // rows)
            def _(r):
                at = pl.ds(pl.multiple_of(r * rows, rows), rows)
                pbuf[k, at, :] = (pbuf[k, at, :].astype(F32) + pa[xx, at, :].astype(F32)).astype(BF16)

            send_b(l, dx).start()
        out_block(l, g, c)

    def finish(l, between):
        send_a(l, g).wait_recv()
        for dx in range(1, G):
            send_b(l, dx).wait_recv()
            if dx == 1:
                between()

        @pl.loop(0, Tk // rows)
        def _(r):
            at = pl.ds(pl.multiple_of(r * rows, rows), rows)
            total = pbuf[me, at, :].astype(F32) + pa[g, at, :].astype(F32)
            for dx in range(1, G):
                total += pb[dx - 1, at, :].astype(F32)
            mixed[at, :] = total
            power = jnp.sum(total * total, axis=1, keepdims=True)
            pw[0, :, at] = jnp.transpose(jnp.broadcast_to(power, (rows, 128)))[0:8, :]

        for d in range(1, TP):
            send_p(l, d).start()
        for d in range(1, TP):
            send_p(l, d).wait_recv()
        for d in range(1, TP):
            send_p(l, d).wait_send()
        for xx in range(G):
            send_a(l, xx).wait_send()
        for dx in range(1, G):
            send_b(l, dx).wait_send()

        @pl.loop(0, Tk // rows)
        def _(r):
            at = pl.ds(pl.multiple_of(r * rows, rows), rows)
            power = pw[0, :, at]
            for d in range(1, TP):
                power += pw[d, :, at]
            power = jnp.transpose(jnp.broadcast_to(power[0:1, :], (128, rows)))[:, 0:1]
            scale = lax.rsqrt(power / D + eps)
            new = xbuf[me, at, :].astype(F32) + mixed[at, :] * scale * post[l : l + 1, :]
            if l == L - 1:
                out_ref[at, :] = new.astype(BF16)
            else:
                xbuf[me, at, :] = new.astype(BF16)

    first = pltpu.make_async_copy(h_ref, xbuf.at[me], xsem)
    first.start()
    exchanged = 0
    tau = -1
    last_tau = begins[-1] + Z - 1

    def advance_to(upto):
        nonlocal tau, exchanged
        while tau < min(upto, last_tau):
            tau += 1
            while exchanged < items and begins[exchanged] <= tau + 2:
                exchange(exchanged)
                exchanged += 1
            advance(tau)

    advance_to(0)
    gather_start(0, h_ref)
    advance_to(1)
    first.wait()
    gather_end(0, h_ref, lambda: advance_to(2))
    advance_to(3)
    norm(0)
    for l in range(L):
        base = 4 * l
        advance_to(begins[base + 2] + Z - 1)
        up(l)
        conv(l)
        advance_to(begins[base + 3] + Z - 1)
        down(l)
        finish(l, lambda: advance_to(base + 4 + Z - 1))
        if l < L - 1:
            gather_start(l + 1, xbuf.at[me])
            advance_to(base + 5 + Z - 1)
            gather_end(l + 1, xbuf.at[me], lambda: advance_to(base + 6 + Z - 1))
            norm(l + 1)

    for i in range(items):
        for h in range(Z - 1):
            @pl.when((z < Z - 1) & (z - h >= 0))
            def _():
                to_right(i, h).wait_send()

            @pl.when((z > 0) & (z + h <= Z - 1))
            def _():
                to_left(i, h).wait_send()

        for d in range(1, Y):
            across(i, d).wait_send()


def solution(mesh):
    SP, TP = mesh.shape["sp"], mesh.shape["tp"]

    def local(hidden_states, pre_gain, post_gain, w_value, w_outer, w_inner, taps, w_out):
        Tk, Dt = hidden_states.shape
        L, Ds, Ct = w_value.shape
        Y, Z, X = layout(SP, TP, Ct)
        G, Cv = X * Y, Ct // Y
        items = 4 * L
        dma = pltpu.SemaphoreType.DMA
        vmem = pl.BlockSpec(memory_space=pltpu.VMEM)
        hbm = pl.BlockSpec(memory_space=pltpu.HBM)
        return pl.pallas_call(
            functools.partial(kernel, SP, TP),
            out_shape=jax.ShapeDtypeStruct((Tk, Dt), BF16),
            in_specs=[hbm, vmem, vmem, hbm, hbm, hbm, vmem, hbm],
            out_specs=vmem,
            scratch_shapes=[
                pltpu.VMEM((L, 3, SP * Ds, Cv), BF16),
                pltpu.VMEM((L, SP * Cv, Ds), BF16),
                pltpu.VMEM((G * 2, Tk, Dt), BF16),
                pltpu.VMEM((Y * Tk, Dt * TP), BF16),
                pltpu.VMEM((G * 2, Tk, Dt), BF16),
                pltpu.VMEM((G, Tk, Dt), BF16),
                pltpu.VMEM((max(G - 1, 1), Tk, Dt), BF16),
                pltpu.VMEM((Tk, Dt), F32),
                pltpu.VMEM((Y * Tk, Cv), BF16),
                pltpu.VMEM((Y * Tk, Cv), F32),
                pltpu.VMEM((L, HALO, Cv), BF16),
                pltpu.VMEM((Y * Tk, Cv), BF16),
                pltpu.VMEM((TP, 8, Tk), F32),
                dma((items,)),
                dma((items, Z)), dma((items, Z)),
                dma((items, Z)), dma((items, Z)),
                dma((items, Y)), dma((items, Y)),
                dma((L, G)), dma((L, G)),
                dma((L, G)), dma((L, G)),
                dma((L, G)), dma((L, G)),
                dma((L, G)), dma((L, G)),
                dma((L, TP)), dma((L, TP)),
                dma((L,)), dma((L,)),
                dma,
            ],
            compiler_params=pltpu.CompilerParams(
                collective_id=0, has_side_effects=True, vmem_limit_bytes=67043328
            ),
        )(hidden_states, pre_gain, post_gain, w_value, w_outer, w_inner, taps, w_out)

    placed = (
        P("sp", "tp"),
        P(),
        P(None, "tp"),
        P(None, "sp", "tp"),
        P(None, "sp", "tp"),
        P(None, "sp", "tp"),
        P(None, None, "tp"),
        P(None, "tp", "sp"),
    )
    return jax.shard_map(
        local, mesh=mesh, in_specs=placed, out_specs=P("sp", "tp"), check_vma=False
    )
```

```python
import functools

import jax
import jax.numpy as jnp
from jax import lax
from jax.experimental import pallas as pl
from jax.experimental.pallas import tpu as pltpu
from jax.sharding import PartitionSpec as P

MESH = pl.DeviceIdType.MESH
HALO = 16
eps = 1e-06
F32 = jnp.float32
BF16 = jnp.bfloat16


def layout(SP, TP, Ct):
    Y = 2 if SP % 2 == 0 and Ct % 256 == 0 else 1
    return Y, SP // Y, TP // 2


def kernel(
    SP, TP, h_ref, pre, post, wv, wo, wi, taps, wout, out_ref,
    wbuf, obuf, xbuf, nbuf, pbuf, pa, pb, mixed, gbuf, oubuf, hbuf, cbuf, pw,
    own_sem, sR, rR, sL, rL, sY, rY, sX, rX, sXr, rXr, sA, rA, sB, rB, sP, rP, sH, rH, xsem,
):
    Y, Z, X = layout(SP, TP, wv.shape[2])
    G = Y * X
    s = lax.axis_index("sp")
    t = lax.axis_index("tp")
    z, y = s // Y, s % Y
    x, c = t // 2, t % 2
    L, Ds, Ct = wv.shape
    Cv = Ct // Y
    Tk, Dt = h_ref.shape
    g = y * X + x
    D = Dt * TP
    items = 4 * L
    wrefs = (wi, wv, wo, wout)

    def rcopy(src, dst, ss, rs, dev):
        return pltpu.make_async_remote_copy(
            src_ref=src, dst_ref=dst, send_sem=ss, recv_sem=rs, device_id=dev, device_id_type=MESH
        )

    barrier = pltpu.get_barrier_semaphore()

    def hello(dev):
        pl.semaphore_signal(barrier, inc=1, device_id=dev, device_id_type=MESH)

    for by in (Y, SP - Y):
        hello(((s + by) % SP, t))
    for dy in range(Y):
        for d in range(TP):
            if dy or d:
                hello((z * Y + (y + dy) % Y, (t + d) % TP))
    pl.semaphore_wait(barrier, 2 + Y * TP - 1)

    def slot(i, b, n):
        l, m = divmod(i, 4)
        if m < 3:
            return wbuf.at[l, m, pl.ds(pl.multiple_of(b * Ds, Ds), n * Ds)]
        return obuf.at[l, pl.ds(pl.multiple_of(b * Cv, Cv), n * Cv)]

    def part(i, yy):
        l, m = divmod(i, 4)
        at = pl.ds(pl.multiple_of(yy * Cv, Cv), Cv)
        return wrefs[m].at[l, :, at] if m < 3 else wrefs[m].at[l, at]

    def to_right(i, h):
        b = slot(i, (z - h) * Y, Y)
        return rcopy(b, b, sR.at[i, h], rR.at[i, h], (s + Y, t))

    def to_left(i, h):
        b = slot(i, (z + h) * Y, Y)
        return rcopy(b, b, sL.at[i, h], rL.at[i, h], (s - Y, t))

    def from_left(i, h):
        b = slot(i, (z - 1 - h) * Y, Y)
        return rcopy(b, b, sR.at[i, h], rR.at[i, h], (s - Y, t))

    def from_right(i, h):
        b = slot(i, (z + 1 + h) * Y, Y)
        return rcopy(b, b, sL.at[i, h], rL.at[i, h], (s + Y, t))

    def across(i, d):
        yy = (y + d) % Y
        return rcopy(part(i, yy), slot(i, s, 1), sY.at[i, d], rY.at[i, d], (z * Y + yy, t))

    def from_across(i, d):
        b = slot(i, z * Y + (y - d + Y) % Y, 1)
        return rcopy(b, b, sY.at[i, d], rY.at[i, d], (z * Y + (y + d) % Y, t))

    def own_copy(i):
        return pltpu.make_async_copy(part(i, y), slot(i, s, 1), own_sem.at[i])

    def exchange(i):
        own_copy(i).start()
        for d in range(1, Y):
            across(i, d).start()

    def stage(i, h):
        if h == 0:
            own_copy(i).wait()
            for d in range(1, Y):
                from_across(i, d).wait_recv()

            @pl.when(z < Z - 1)
            def _():
                to_right(i, 0).start()

            @pl.when(z > 0)
            def _():
                to_left(i, 0).start()

            return

        @pl.when(z - h >= 0)
        def _():
            from_left(i, h - 1).wait_recv()
            if h <= Z - 2:
                @pl.when(z < Z - 1)
                def _():
                    to_right(i, h).start()

        @pl.when(z + h <= Z - 1)
        def _():
            from_right(i, h - 1).wait_recv()
            if h <= Z - 2:
                @pl.when(z > 0)
                def _():
                    to_left(i, h).start()

    begins = list(range(items))

    def advance(tau, skip=-1):
        for i in range(items):
            if i != skip and 0 <= tau - begins[i] <= Z - 1:
                stage(i, tau - begins[i])

    mate = (s, x * 2 + 1 - c)

    def dev(gg, cc):
        return (z * Y + gg // X, (gg % X) * 2 + cc)

    me = g * 2 + c

    def x_mate(l, src):
        return rcopy(src, xbuf.at[me], sX.at[l, 0], rX.at[l, 0], mate)

    def x_far(l, d, src):
        return rcopy(src, xbuf.at[me], sX.at[l, d], rX.at[l, d], dev((g + d) % G, c))

    def x_relay(l, d):
        b = xbuf.at[((g - d + G) % G) * 2 + c]
        return rcopy(b, b, sXr.at[l, d], rXr.at[l, d], mate)

    def gather_start(l, src):
        for d in range(1, G):
            x_far(l, d, src).start()
        x_mate(l, src).start()

    def gather_end(l, src, between):
        for d in range(1, G):
            b = xbuf.at[((g - d + G) % G) * 2 + c]
            rcopy(b, b, sX.at[l, d], rX.at[l, d], mate).wait_recv()
            x_relay(l, d).start()
            if d == 1:
                between()
        b = xbuf.at[g * 2 + 1 - c]
        rcopy(b, b, sX.at[l, 0], rX.at[l, 0], mate).wait_recv()
        for d in range(1, G):
            b = xbuf.at[((g - d + G) % G) * 2 + 1 - c]
            rcopy(b, b, sXr.at[l, d], rXr.at[l, d], mate).wait_recv()
        x_mate(l, src).wait_send()
        for d in range(1, G):
            x_far(l, d, src).wait_send()
            x_relay(l, d).wait_send()

    rows = 128 if Tk % 128 == 0 else Tk

    def norm(l):
        for yy in range(Y):
            @pl.loop(0, Tk // rows)
            def _(r):
                at = pl.ds(pl.multiple_of(r * rows, rows), rows)
                to = pl.ds(pl.multiple_of(yy * Tk + r * rows, rows), rows)
                total = jnp.zeros((rows, 1), F32)
                for k in range(TP):
                    v = xbuf[yy * TP + k, at, :].astype(F32)
                    total += jnp.sum(v * v, axis=1, keepdims=True)
                scale = lax.rsqrt(total / D + eps)
                for k in range(TP):
                    cols = slice(k * Dt, (k + 1) * Dt)
                    v = xbuf[yy * TP + k, at, :].astype(F32)
                    nbuf[to, cols] = (v * scale * pre[l : l + 1, cols]).astype(BF16)

    def up_gate(l):
        @pl.loop(0, Y)
        def _(j):
            at = pl.ds(pl.multiple_of(j * Tk, Tk), Tk)
            inner = jnp.dot(nbuf[at, :], wbuf[l, 0], preferred_element_type=F32)
            value = jnp.dot(nbuf[at, :], wbuf[l, 1], preferred_element_type=F32)
            gbuf[at, :] = (inner * value).astype(BF16)

    def up_outer(l):
        @pl.loop(0, Y)
        def _(j):
            at = pl.ds(pl.multiple_of(j * Tk, Tk), Tk)
            oubuf[at, :] = jnp.dot(nbuf[at, :], wbuf[l, 2], preferred_element_type=F32)

    def halo(l, dev):
        return rcopy(gbuf.at[pl.ds(Y * Tk - HALO, HALO)], hbuf.at[l], sH.at[l], rH.at[l], dev)

    def halo_start(l):
        @pl.when(z < Z - 1)
        def _():
            halo(l, (s + Y, t)).start()

    def conv(l):
        @pl.when(z > 0)
        def _():
            halo(l, (s - Y, t)).wait_recv()

        @pl.when(z == 0)
        def _():
            hbuf[l] = jnp.zeros((HALO, Cv), BF16)

        @pl.loop(0, Cv // 128)
        def _(j):
            cols = pl.ds(pl.multiple_of(j * 128, 128), 128)
            mine = pl.ds(pl.multiple_of(y * Cv + j * 128, 128), 128)
            v = gbuf[:, cols].astype(F32)
            before = hbuf[l, :, cols].astype(F32)
            last, prev = before[HALO - 1 : HALO, :], before[HALO - 2 : HALO - 1, :]
            at = lax.broadcasted_iota(jnp.int32, v.shape, 0)
            g1 = jnp.where(at == 0, last, pltpu.roll(v, 1, 0))
            g2 = jnp.where(at == 0, prev, jnp.where(at == 1, last, pltpu.roll(v, 2, 0)))
            conv = g2 * taps[l, 0:1, mine] + g1 * taps[l, 1:2, mine] + v * taps[l, 2:3, mine]
            cbuf[:, cols] = (oubuf[:, cols] * conv).astype(BF16)

        @pl.when(z < Z - 1)
        def _():
            halo(l, (s + Y, t)).wait_send()

    nb = Dt // Ds

    def out_block(l, gg, cc):
        yy, tt = gg // X, (gg % X) * 2 + cc
        at = pl.ds(pl.multiple_of(yy * Tk, Tk), Tk)
        for b in range(nb):
            of = pl.ds(pl.multiple_of((tt * nb + b) * Cv, Cv), Cv)
            pbuf[gg * 2 + cc, :, b * Ds : (b + 1) * Ds] = jnp.dot(
                cbuf[at, :], obuf[l, of, :], preferred_element_type=F32
            ).astype(BF16)

    def send_a(l, xx):
        return rcopy(pbuf.at[xx * 2 + 1 - c], pa.at[xx], sA.at[l, xx], rA.at[l, xx], mate)

    def send_b(l, dx):
        gg = (g + dx) % G
        return rcopy(pbuf.at[gg * 2 + c], pb.at[dx - 1], sB.at[l, dx], rB.at[l, dx], dev(gg, c))

    def send_p(l, d):
        return rcopy(pw.at[0], pw.at[d], sP.at[l, d], rP.at[l, d], (s, (t + d) % TP))

    def down(l):
        for dx in range(1, G + 1):
            xx = (g + dx) % G
            out_block(l, xx, 1 - c)
            send_a(l, xx).start()
        for dx in range(1, G):
            xx = (g + dx) % G
            k = xx * 2 + c
            out_block(l, xx, c)
            send_a(l, xx).wait_recv()

            @pl.loop(0, Tk // rows)
            def _(r):
                at = pl.ds(pl.multiple_of(r * rows, rows), rows)
                pbuf[k, at, :] = (pbuf[k, at, :].astype(F32) + pa[xx, at, :].astype(F32)).astype(BF16)

            send_b(l, dx).start()
        out_block(l, g, c)

    by_block = SP == Y * TP

    def down_block(l, tt):
        cc = tt % 2
        for yy in range(Y):
            gg = yy * X + tt // 2
            out_block(l, gg, cc)

            @pl.when(cc != c)
            def _():
                send_a(l, gg).start()

            @pl.when(cc == c)
            def _():
                send_a(l, gg).wait_recv()

                @pl.when(gg != g)
                def _():
                    @pl.loop(0, Tk // rows)
                    def _(r):
                        at = pl.ds(pl.multiple_of(r * rows, rows), rows)
                        k = gg * 2 + c
                        pbuf[k, at, :] = (pbuf[k, at, :].astype(F32) + pa[gg, at, :].astype(F32)).astype(BF16)

                    send_b(l, (gg - g + G) % G).start()

    def down_step(l, h):
        if h == 0:
            down_block(l, z)
            return

        @pl.when(z - h >= 0)
        def _():
            down_block(l, z - h)

        @pl.when(z + h <= Z - 1)
        def _():
            down_block(l, z + h)

    def finish(l, between):
        if not by_block:
            send_a(l, g).wait_recv()
        for dx in range(1, G):
            send_b(l, dx).wait_recv()
            if dx == 1:
                between()

        @pl.loop(0, Tk // rows)
        def _(r):
            at = pl.ds(pl.multiple_of(r * rows, rows), rows)
            total = pbuf[me, at, :].astype(F32) + pa[g, at, :].astype(F32)
            for dx in range(1, G):
                total += pb[dx - 1, at, :].astype(F32)
            mixed[at, :] = total
            power = jnp.sum(total * total, axis=1, keepdims=True)
            pw[0, :, at] = jnp.transpose(jnp.broadcast_to(power, (rows, 128)))[0:8, :]

        for d in range(1, TP):
            send_p(l, d).start()
        for d in range(1, TP):
            send_p(l, d).wait_recv()
        for d in range(1, TP):
            send_p(l, d).wait_send()
        for xx in range(G):
            send_a(l, xx).wait_send()
        for dx in range(1, G):
            send_b(l, dx).wait_send()

        @pl.loop(0, Tk // rows)
        def _(r):
            at = pl.ds(pl.multiple_of(r * rows, rows), rows)
            power = pw[0, :, at]
            for d in range(1, TP):
                power += pw[d, :, at]
            power = jnp.transpose(jnp.broadcast_to(power[0:1, :], (128, rows)))[:, 0:1]
            scale = lax.rsqrt(power / D + eps)
            new = xbuf[me, at, :].astype(F32) + mixed[at, :] * scale * post[l : l + 1, :]
            if l == L - 1:
                out_ref[at, :] = new.astype(BF16)
            else:
                xbuf[me, at, :] = new.astype(BF16)

    first = pltpu.make_async_copy(h_ref, xbuf.at[me], xsem)
    first.start()
    exchanged = 0
    tau = -1
    last_tau = begins[-1] + Z - 1

    def advance_to(upto, skip=-1):
        nonlocal tau, exchanged
        while tau < min(upto, last_tau):
            tau += 1
            while exchanged < items and begins[exchanged] <= tau + 2:
                exchange(exchanged)
                exchanged += 1
            advance(tau, skip)

    advance_to(0)
    gather_start(0, h_ref)
    advance_to(1)
    first.wait()
    gather_end(0, h_ref, lambda: advance_to(2))
    advance_to(3)
    norm(0)
    for l in range(L):
        base = 4 * l
        advance_to(begins[base + 1] + Z - 1)
        up_gate(l)
        halo_start(l)
        late = base + 3 if l == L - 1 and by_block and Z > 2 else -1
        advance_to(begins[base + 2] + Z - 1, late)
        if late >= 0:
            @pl.when((z > 0) & (z < Z - 1))
            def _():
                stage(late, Z - 2)

        up_outer(l)
        conv(l)
        if by_block:
            for h in range(Z - 2):
                down_step(l, h)
            if late >= 0:
                @pl.when((z == 0) | (z == Z - 1))
                def _():
                    stage(late, Z - 2)

            if Z > 1:
                down_step(l, Z - 2)
            advance_to(begins[base + 3] + Z - 1)
            down_step(l, Z - 1)
        else:
            advance_to(begins[base + 3] + Z - 1)
            down(l)
        finish(l, lambda: advance_to(base + 4 + Z - 1))
        if l < L - 1:
            gather_start(l + 1, xbuf.at[me])
            gather_end(l + 1, xbuf.at[me], lambda: advance_to(base + 5 + Z - 1))
            norm(l + 1)

    for i in range(items):
        for h in range(Z - 1):
            @pl.when((z < Z - 1) & (z - h >= 0))
            def _():
                to_right(i, h).wait_send()

            @pl.when((z > 0) & (z + h <= Z - 1))
            def _():
                to_left(i, h).wait_send()

        for d in range(1, Y):
            across(i, d).wait_send()


def solution(mesh):
    SP, TP = mesh.shape["sp"], mesh.shape["tp"]

    def local(hidden_states, pre_gain, post_gain, w_value, w_outer, w_inner, taps, w_out):
        Tk, Dt = hidden_states.shape
        L, Ds, Ct = w_value.shape
        Y, Z, X = layout(SP, TP, Ct)
        G, Cv = X * Y, Ct // Y
        items = 4 * L
        dma = pltpu.SemaphoreType.DMA
        vmem = pl.BlockSpec(memory_space=pltpu.VMEM)
        hbm = pl.BlockSpec(memory_space=pltpu.HBM)
        return pl.pallas_call(
            functools.partial(kernel, SP, TP),
            out_shape=jax.ShapeDtypeStruct((Tk, Dt), BF16),
            in_specs=[hbm, vmem, vmem, hbm, hbm, hbm, vmem, hbm],
            out_specs=vmem,
            scratch_shapes=[
                pltpu.VMEM((L, 3, SP * Ds, Cv), BF16),
                pltpu.VMEM((L, SP * Cv, Ds), BF16),
                pltpu.VMEM((G * 2, Tk, Dt), BF16),
                pltpu.VMEM((Y * Tk, Dt * TP), BF16),
                pltpu.VMEM((G * 2, Tk, Dt), BF16),
                pltpu.VMEM((G, Tk, Dt), BF16),
                pltpu.VMEM((max(G - 1, 1), Tk, Dt), BF16),
                pltpu.VMEM((Tk, Dt), F32),
                pltpu.VMEM((Y * Tk, Cv), BF16),
                pltpu.VMEM((Y * Tk, Cv), F32),
                pltpu.VMEM((L, HALO, Cv), BF16),
                pltpu.VMEM((Y * Tk, Cv), BF16),
                pltpu.VMEM((TP, 8, Tk), F32),
                dma((items,)),
                dma((items, Z)), dma((items, Z)),
                dma((items, Z)), dma((items, Z)),
                dma((items, Y)), dma((items, Y)),
                dma((L, G)), dma((L, G)),
                dma((L, G)), dma((L, G)),
                dma((L, G)), dma((L, G)),
                dma((L, G)), dma((L, G)),
                dma((L, TP)), dma((L, TP)),
                dma((L,)), dma((L,)),
                dma,
            ],
            compiler_params=pltpu.CompilerParams(
                collective_id=0, has_side_effects=True, vmem_limit_bytes=67043328
            ),
        )(hidden_states, pre_gain, post_gain, w_value, w_outer, w_inner, taps, w_out)

    placed = (
        P("sp", "tp"),
        P(),
        P(None, "tp"),
        P(None, "sp", "tp"),
        P(None, "sp", "tp"),
        P(None, "sp", "tp"),
        P(None, None, "tp"),
        P(None, "tp", "sp"),
    )
    return jax.shard_map(
        local, mesh=mesh, in_specs=placed, out_specs=P("sp", "tp"), check_vma=False
    )
```
